32 devices in a mesh: kv: 8 (over z, x), tp: 4 (over y, core).
Axes of the slice: x: 2, y: 2, z: 4, core: 2. Of those that a mesh axis runs over, the one named last changes fastest.
Arguments:
- hidden: bfloat16 [512, 4096], P(None, 'kv'), as said below
- norm_gain: bfloat16 [4096], replicated, may hold values from 0.099609375 to 1.8984375
- w_query: bfloat16 [4096, 4096], P('kv', 'tp'), may hold values from -0.09375 to 0.09375
- w_key: bfloat16 [4096, 4096], P('kv', 'tp'), may hold values from -0.09375 to 0.09375
- w_value: bfloat16 [4096, 8192], P('kv', 'tp'), may hold values from -0.09375 to 0.09375
- w_gate: bfloat16 [4096, 8192], P('kv', 'tp'), may hold values from -0.09375 to 0.09375
- w_write: bfloat16 [4096, 32], P('kv', 'tp'), may hold values from -0.09375 to 0.09375
- w_decay: bfloat16 [4096, 32], P('kv', 'tp'), may hold values from -0.09375 to 0.09375
- w_out: bfloat16 [8192, 4096], P('tp', 'kv'), may hold values from -0.0625 to 0.0625
- decay_rate: float32 [32], P('tp'), may hold values from 0 to 4, as said below
- head_gain: float32 [256], replicated, may hold values from 0.1 to 1.9
- carried_state: float32 [128, 32, 128, 256], P('kv', 'tp'), may hold values from -4 to 4
- last_keys: bfloat16 [128, 4, 4096], P('kv', None, 'tp'), may hold values from -6 to 6
- last_values: bfloat16 [128, 4, 8192], P('kv', None, 'tp'), may hold values from -6 to 6
- last_writes: float32 [128, 4, 32], P('kv', None, 'tp'), may hold values from -6 to 6
- last_decays: float32 [128, 4, 32], P('kv', None, 'tp'), may hold values from -6 to 6
- accepted: int32 [128], P('kv'), may hold values from 0 to 4
Outputs:
- mixed_out: bfloat16 [512, 4096], P('tp', 'kv')
- committed: float32 [128, 32, 128, 256], P('kv', 'tp')
The draws below stay inside these ranges and needn't reach their ends.
Inputs may be any that keep to these rules, and one draw needn't show every extreme that they name: `decay_rate`: positive. `hidden`: finite real values.
All inputs are finite; a program needn't handle non-finite values.
Results may differ from the reference program's by a relative error of at most 0.029.
Values may be sent and summed in bfloat16 or wider, within the bound.
No kernel may reach another device: no remote copies, remote signals or barrier semaphores. Data moves between devices by JAX's collectives and lax.ppermute only.
A program may use at most 128 MiB of HBM per device.

```python
import math
import jax
import jax.numpy as jnp
from jax import lax

D = 4096
HEADS = 32
DK = 128
DV = 256
PROP = 4
SEQS = 128
TOKENS = 512
N_TP = 4


def draw_hidden(key, part):
    first, second, third = jax.random.split(key, 3)
    group = max(D // 16, 1)
    groups = (D + group - 1) // group
    scales = jnp.exp(jax.random.uniform(first, (groups,), jnp.float32, math.log(0.25), math.log(4.0)))
    channel_scale = scales[jnp.arange(D) // group]
    base = jax.random.normal(second, (TOKENS, D), jnp.float32)
    return (base * channel_scale[None, :]).astype(jnp.bfloat16)


def draw_decay_rate(key, part):
    return jnp.exp(jax.random.uniform(key, (HEADS,), jnp.float32, math.log(0.02), math.log(4.0)))


def with_ends(entries, own_key, smallest, largest):
    dims = entries.shape
    spot = [jax.random.randint(jax.random.fold_in(own_key, axis), (), 0, dims[axis]) for axis in range(len(dims))]
    entries = entries.at[tuple(spot)].set(smallest)
    longest = dims.index(max(dims))
    spot[longest] = (spot[longest] + 1) % dims[longest]
    return entries.at[tuple(spot)].set(largest)


def steps_of(rng, extent, cuts, low, top_value):
    loudness = 1.0
    for axis_at, shards_of in cuts:
        draws = jax.random.uniform(jax.random.fold_in(jax.random.fold_in(rng, 6), axis_at), (shards_of,), jnp.float32, low / len(cuts), top_value / len(cuts))
        loudness = loudness * jnp.repeat(jnp.exp(draws), extent[axis_at] // shards_of).reshape((-1,) + (1,) * (len(extent) - 1 - axis_at))
    return loudness


def gaussian(stream_key, dims, deviation, most, cuts=(), held_as=jnp.bfloat16):
    array = jax.random.normal(stream_key, dims, jnp.float32) * deviation
    if len(cuts) > 0:
        array = steps_of(stream_key, dims, cuts, -0.22, 0.18) * array
    return jnp.clip(array, min=-most, max=most).astype(held_as)


def setup_inputs(seed: int = 0) -> dict:
    streams_of = jax.random.split(jax.random.key(seed), 18)
    return {
        "hidden": draw_hidden(jax.random.fold_in(streams_of[17], 71), 0),
        "norm_gain": jnp.clip(1.0 + 0.18 * jax.random.normal(streams_of[1], (D,), jnp.float32), 0.099609375, 1.8984375).astype(jnp.bfloat16),
        "w_query": gaussian(streams_of[2], (D, HEADS * DK), D ** -0.5, 0.09375, ((0, 8), (1, 4))),
        "w_key": gaussian(streams_of[3], (D, HEADS * DK), D ** -0.5, 0.09375, ((0, 8), (1, 4))),
        "w_value": gaussian(streams_of[4], (D, HEADS * DV), D ** -0.5, 0.09375, ((0, 8), (1, 4))),
        "w_gate": gaussian(streams_of[5], (D, HEADS * DV), D ** -0.5, 0.09375, ((0, 8), (1, 4))),
        "w_write": gaussian(streams_of[6], (D, HEADS), D ** -0.5, 0.09375, ((0, 8), (1, 4))),
        "w_decay": gaussian(streams_of[7], (D, HEADS), D ** -0.5, 0.09375, ((0, 8), (1, 4))),
        "w_out": gaussian(streams_of[8], (HEADS * DV, D), (HEADS * DV) ** -0.5, 0.0625, ((0, 4), (1, 8))),
        "decay_rate": draw_decay_rate(jax.random.fold_in(streams_of[17], 71), 0),
        "head_gain": jnp.clip(1.0 + 0.18 * jax.random.normal(streams_of[10], (DV,), jnp.float32), 0.1, 1.9),
        "carried_state": gaussian(streams_of[11], (SEQS, HEADS, DK, DV), 0.3, 4.0, ((0, 8), (1, 4)), jnp.float32),
        "last_keys": gaussian(streams_of[12], (SEQS, PROP, HEADS * DK), 1.0, 6.0, ((0, 8), (2, 4))),
        "last_values": gaussian(streams_of[13], (SEQS, PROP, HEADS * DV), 1.0, 6.0, ((0, 8), (2, 4))),
        "last_writes": gaussian(streams_of[14], (SEQS, PROP, HEADS), 1.0, 6.0, ((0, 8), (2, 4)), jnp.float32),
        "last_decays": gaussian(streams_of[15], (SEQS, PROP, HEADS), 1.0, 6.0, ((0, 8), (2, 4)), jnp.float32),
        "accepted": with_ends(jax.random.randint(streams_of[16], (SEQS,), 0, PROP + 1), jax.random.fold_in(streams_of[16], 1), 0, PROP).astype(jnp.int32),
    }


norm_eps = 1e-06
highest = lax.Precision.HIGHEST

def unit_rows(matrix):
    return matrix * lax.rsqrt(lax.optimization_barrier(jnp.sum(matrix * matrix, -1, keepdims=True)) + norm_eps)

def corrected(key_rows, values, write_rate, log_decay, start_state):
    proposals = key_rows.shape[2]
    value_width = values.shape[-1]
    running = jnp.cumsum(log_decay, axis=-1)
    causal = jnp.tril(jnp.ones((proposals, proposals), dtype=bool))
    spread = running[..., :, None] - running[..., None, :]
    weights = jnp.where(causal, jnp.exp(jnp.where(causal, spread, 0.0)), 0.0)
    strong_keys = key_rows * write_rate[..., None]
    lower_part = jnp.einsum('bhcd,bhsd->bhcs', strong_keys, key_rows, precision=highest)
    lower_part = lower_part * weights * (1.0 - jnp.eye(proposals, dtype=jnp.float32))
    right_side = jnp.concatenate([values * write_rate[..., None], strong_keys * jnp.exp(running)[..., None]], -1)
    solved_rows = []
    for later in range(proposals):
        current = right_side[..., later, :]
        for early in range(later):
            current = current - lower_part[..., later, early, None] * solved_rows[early]
        solved_rows.append(current)
    solved = jnp.stack(solved_rows, axis=2)
    fresh_values = solved[..., :value_width] - jnp.einsum('bhcd,bhde->bhce', solved[..., value_width:], start_state, precision=highest)
    return (fresh_values, running, weights)

def advance(key_rows, fresh_values, running, start_state):
    tail_decay = jnp.exp(running[..., -1:] - running)
    return start_state * jnp.exp(running[..., -1])[..., None, None] + jnp.einsum('bhcd,bhce->bhde', key_rows * tail_decay[..., None], fresh_values, precision=highest)

def readout(queries, key_rows, fresh_values, running, weights, start_state):
    scores = jnp.einsum('bhcd,bhsd->bhcs', queries, key_rows, precision=highest) * weights
    carried = jnp.einsum('bhcd,bhde->bhce', queries * jnp.exp(running)[..., None], start_state, precision=highest)
    return carried + jnp.einsum('bhcs,bhse->bhce', scores, fresh_values, precision=highest)

def core(proj_query, proj_key, proj_value, proj_gate, proj_write, proj_decay, decay_rate, head_gain, carried_state, last_keys, last_values, last_writes, last_decays, accepted):
    seq_count, head_count, key_width, value_width = carried_state.shape
    proposals = last_keys.shape[1]

    def by_head(matrix, width):
        return jnp.transpose(matrix.reshape(seq_count, proposals, head_count, width), (0, 2, 1, 3))

    def by_head_small(matrix):
        return jnp.transpose(matrix.reshape(seq_count, proposals, head_count), (0, 2, 1))
    rates = decay_rate.astype(jnp.float32)[None, :, None]
    taken = (jnp.arange(proposals, dtype=jnp.int32)[None, :] < accepted[:, None]).astype(jnp.float32)[:, None, :]
    old_keys = unit_rows(by_head(last_keys.astype(jnp.float32), key_width))
    old_values = by_head(last_values.astype(jnp.float32), value_width)
    old_write = jax.nn.sigmoid(by_head_small(last_writes)) * taken
    old_decay = -rates * jax.nn.softplus(by_head_small(last_decays)) * taken
    fresh_values, running, weights = corrected(old_keys, old_values, old_write, old_decay, carried_state)
    committed = advance(old_keys, fresh_values, running, carried_state)
    queries = unit_rows(by_head(jax.nn.silu(proj_query), key_width)) * key_width ** (-0.5)
    key_rows = unit_rows(by_head(jax.nn.silu(proj_key), key_width))
    values = by_head(jax.nn.silu(proj_value), value_width)
    write_rate = jax.nn.sigmoid(by_head_small(proj_write))
    log_decay = -rates * jax.nn.softplus(by_head_small(proj_decay))
    fresh_values, running, weights = corrected(key_rows, values, write_rate, log_decay, committed)
    result = readout(queries, key_rows, fresh_values, running, weights, committed)
    normed = result * lax.rsqrt(lax.optimization_barrier(jnp.mean(result * result, -1, keepdims=True)) + norm_eps) * head_gain.astype(jnp.float32)
    gated = normed * jax.nn.silu(by_head(proj_gate, value_width))
    gated_rows = jnp.transpose(gated, (0, 2, 1, 3)).reshape(seq_count * proposals, head_count * value_width).astype(jnp.bfloat16)
    return (gated_rows, committed)

def reference(hidden, norm_gain, w_query, w_key, w_value, w_gate, w_write, w_decay, w_out, decay_rate, head_gain, carried_state, last_keys, last_values, last_writes, last_decays, accepted):
    wide_rows = hidden.astype(jnp.float32)
    inverse = lax.rsqrt(lax.optimization_barrier(jnp.sum(wide_rows * wide_rows, -1, keepdims=True)) / D + norm_eps)
    scaled = (wide_rows * norm_gain.astype(jnp.float32)).astype(jnp.bfloat16)

    def project(weight):
        return jnp.dot(scaled, weight, preferred_element_type=jnp.float32) * inverse
    gated_rows, committed = core(project(w_query), project(w_key), project(w_value), project(w_gate), project(w_write), project(w_decay), decay_rate, head_gain, carried_state, last_keys, last_values, last_writes, last_decays, accepted)
    grouped = gated_rows.astype(jnp.float32).reshape(TOKENS, N_TP, -1)
    weight_groups = w_out.astype(jnp.float32).reshape(N_TP, -1, D)
    partial_value = jnp.einsum('tmc,mcd->mtd', grouped, weight_groups)
    rounded = lax.optimization_barrier(partial_value.astype(jnp.bfloat16)).astype(jnp.float32)
    mixed_out = lax.optimization_barrier(jnp.sum(rounded, 0)).astype(jnp.bfloat16)
    return (mixed_out, committed)
```

```python
import jax
import jax.numpy as jnp
from jax import lax
from jax.sharding import PartitionSpec as P

norm_eps = 1e-06
highest = lax.Precision.HIGHEST


def unit_rows(matrix):
    return matrix * lax.rsqrt(jnp.sum(matrix * matrix, -1, keepdims=True) + norm_eps)


def corrected(key_rows, values, write_rate, log_decay, start_state):
    proposals = key_rows.shape[2]
    value_width = values.shape[-1]
    running = jnp.cumsum(log_decay, axis=-1)
    causal = jnp.tril(jnp.ones((proposals, proposals), dtype=bool))
    spread = running[..., :, None] - running[..., None, :]
    weights = jnp.where(causal, jnp.exp(jnp.where(causal, spread, 0.0)), 0.0)
    strong_keys = key_rows * write_rate[..., None]
    lower_part = jnp.einsum("bhcd,bhsd->bhcs", strong_keys, key_rows, precision=highest)
    lower_part = lower_part * weights * (1.0 - jnp.eye(proposals, dtype=jnp.float32))
    right_side = jnp.concatenate(
        [values * write_rate[..., None], strong_keys * jnp.exp(running)[..., None]], -1
    )
    solved_rows = []
    for later in range(proposals):
        current = right_side[..., later, :]
        for early in range(later):
            current = current - lower_part[..., later, early, None] * solved_rows[early]
        solved_rows.append(current)
    solved = jnp.stack(solved_rows, axis=2)
    fresh_values = solved[..., :value_width] - jnp.einsum(
        "bhcd,bhde->bhce", solved[..., value_width:], start_state, precision=highest
    )
    return (fresh_values, running, weights)


def advance(key_rows, fresh_values, running, start_state):
    tail_decay = jnp.exp(running[..., -1:] - running)
    return start_state * jnp.exp(running[..., -1])[..., None, None] + jnp.einsum(
        "bhcd,bhce->bhde", key_rows * tail_decay[..., None], fresh_values, precision=highest
    )


def plane_of(ranks):
    columns = 2 ** ((ranks.bit_length() - 1) // 2)
    return (ranks // columns, columns)


def rank_pairs(ranks, moves, along_columns):
    lines, columns = plane_of(ranks)
    if along_columns:
        return [
            (line * columns + src, line * columns + dst)
            for line in range(lines)
            for src, dst in moves
        ]
    return [
        (src * columns + column, dst * columns + column)
        for column in range(columns)
        for src, dst in moves
    ]


def take(array, index, dim):
    return lax.dynamic_index_in_dim(array, index, dim, keepdims=False)


def add_up(*arrays):
    total = arrays[0].astype(jnp.float32)
    for array in arrays[1:]:
        total = total + array.astype(jnp.float32)
    return total


def line_sum(blocks, dim, ranks, along_columns):
    size = blocks.shape[dim]
    lines, columns = plane_of(ranks)
    rank = lax.axis_index("kv")
    place = rank % columns if along_columns else rank // columns
    own = take(blocks, place, dim)
    if size == 1:
        return own.astype(jnp.float32)
    if size == 2:
        got = lax.ppermute(
            take(blocks, 1 - place, dim),
            "kv",
            rank_pairs(ranks, [(0, 1), (1, 0)], along_columns),
        )
        return add_up(own, got)
    up = take(blocks, jnp.minimum(size - 1 + place, size - 1), dim)
    down = take(blocks, jnp.maximum(place - size + 1, 0), dim)
    got_up = got_down = None
    for step in range(1, size):
        moves_up = [(src, src + 1) for src in range(step)]
        moves_down = [(size - 1 - src, size - 2 - src) for src in range(step)]
        got_up = lax.ppermute(up, "kv", rank_pairs(ranks, moves_up, along_columns))
        got_down = lax.ppermute(down, "kv", rank_pairs(ranks, moves_down, along_columns))
        if step < size - 1:
            mine = take(blocks, jnp.minimum(size - 1 - step + place, size - 1), dim)
            up = add_up(got_up, mine).astype(jnp.bfloat16)
            mine = take(blocks, jnp.maximum(place - size + 1 + step, 0), dim)
            down = add_up(got_down, mine).astype(jnp.bfloat16)
    return add_up(own, got_up, got_down)


def plane_sum(partial, ranks, columns_first):
    lines, columns = plane_of(ranks)
    rows, width = partial.shape
    blocks = partial.reshape(lines, columns, rows // ranks, width)
    if columns_first:
        blocks = line_sum(blocks, 1, ranks, True).astype(jnp.bfloat16)
        return line_sum(blocks, 0, ranks, False)
    blocks = line_sum(blocks, 0, ranks, False).astype(jnp.bfloat16)
    return line_sum(blocks, 0, ranks, True)


def line_gather(block, ranks, along_columns):
    lines, columns = plane_of(ranks)
    size = columns if along_columns else lines
    parts = {0: block}
    up = down = block
    for step in range(1, size):
        moves_up = [(src, src + 1) for src in range(step - 1, size - 1)]
        moves_down = [(size - 1 - src, size - 2 - src) for src in range(step - 1, size - 1)]
        up = lax.ppermute(up, "kv", rank_pairs(ranks, moves_up, along_columns))
        down = lax.ppermute(down, "kv", rank_pairs(ranks, moves_down, along_columns))
        parts[-step] = up
        parts[step] = down
    return parts


def plane_gather(block, ranks):
    lines, columns = plane_of(ranks)
    rank = lax.axis_index("kv")
    line, column = rank // columns, rank % columns
    parts = line_gather(block, ranks, False)
    near = jnp.stack([parts[d] for d in range(1 - lines, lines)])
    near = lax.dynamic_slice_in_dim(near, lines - 1 - line, lines, 0)
    if columns == 2:
        swap = [(0, 1), (1, 0)]
        far_parts = []
        for d in range(1 - lines, lines):
            holders = [r for r in range(lines) if 0 <= r + d < lines]
            pairs = [
                (r * columns + src, r * columns + dst) for r in holders for src, dst in swap
            ]
            far_parts.append(lax.ppermute(parts[d], "kv", pairs))
        far = lax.dynamic_slice_in_dim(jnp.stack(far_parts), lines - 1 - line, lines, 0)
        first = jnp.where(column == 0, near, far)
        second = jnp.where(column == 0, far, near)
        whole = jnp.stack([first, second], axis=1)
    else:
        parts = line_gather(near, ranks, True)
        whole = jnp.stack([parts[d] for d in range(1 - columns, columns)])
        whole = lax.dynamic_slice_in_dim(whole, columns - 1 - column, columns, 0)
        whole = jnp.swapaxes(whole, 0, 1)
    return whole.reshape(ranks * block.shape[0], block.shape[1])


def by_head(matrix, seq_count, proposals, width):
    return jnp.transpose(matrix.reshape(seq_count, proposals, -1, width), (0, 2, 1, 3))


def by_head_small(matrix, seq_count, proposals):
    return jnp.transpose(matrix.reshape(seq_count, proposals, -1), (0, 2, 1))


def commit(decay_rate, carried_state, last_keys, last_values, last_writes, last_decays, accepted):
    seq_count, head_count, key_width, value_width = carried_state.shape
    proposals = last_keys.shape[1]
    rates = decay_rate[None, :, None]
    taken = (jnp.arange(proposals, dtype=jnp.int32)[None, :] < accepted[:, None]).astype(
        jnp.float32
    )[:, None, :]
    old_keys = unit_rows(by_head(last_keys.astype(jnp.float32), seq_count, proposals, key_width))
    old_values = by_head(last_values.astype(jnp.float32), seq_count, proposals, value_width)
    old_write = jax.nn.sigmoid(by_head_small(last_writes, seq_count, proposals)) * taken
    old_decay = -rates * jax.nn.softplus(by_head_small(last_decays, seq_count, proposals)) * taken
    fresh_values, running, weights = corrected(
        old_keys, old_values, old_write, old_decay, carried_state
    )
    return advance(old_keys, fresh_values, running, carried_state)


def verify_rows(proj_query, proj_key, proj_value, proj_write, proj_decay, decay_rate, state):
    seq_count, head_count, key_width, value_width = state.shape
    proposals = proj_query.shape[0] // seq_count
    rates = decay_rate[None, :, None]
    queries = unit_rows(by_head(jax.nn.silu(proj_query), seq_count, proposals, key_width))
    queries = queries * key_width ** (-0.5)
    key_rows = unit_rows(by_head(jax.nn.silu(proj_key), seq_count, proposals, key_width))
    values = by_head(jax.nn.silu(proj_value), seq_count, proposals, value_width)
    write_rate = jax.nn.sigmoid(by_head_small(proj_write, seq_count, proposals))
    log_decay = -rates * jax.nn.softplus(by_head_small(proj_decay, seq_count, proposals))
    running = jnp.cumsum(log_decay, axis=-1)
    both = jnp.concatenate([key_rows, queries], axis=2)
    carried = jnp.einsum("bhcd,bhde->bhce", both, state, precision=highest)
    carried = carried * jnp.exp(jnp.concatenate([running, running], -1))[..., None]
    inner = jnp.sum(both[:, :, :, None, :] * key_rows[:, :, None, :, :], -1)
    fresh, result = [], []
    for later in range(proposals):
        current = values[:, :, later] - carried[:, :, later]
        read = carried[:, :, proposals + later]
        for early in range(later + 1):
            weight = jnp.exp(running[..., later] - running[..., early])
            if early < later:
                current = current - (inner[..., later, early] * weight)[..., None] * fresh[early]
            else:
                fresh.append(current * write_rate[..., later, None])
            read = read + (inner[..., proposals + later, early] * weight)[..., None] * fresh[early]
        result.append(read)
    return jnp.stack(result, axis=2)


def per_device(
    hidden,
    norm_gain,
    w_query,
    w_key,
    w_value,
    w_gate,
    w_write,
    w_decay,
    w_out,
    decay_rate,
    head_gain,
    carried_state,
    last_keys,
    last_values,
    last_writes,
    last_decays,
    accepted,
):
    ranks = lax.axis_size("kv")
    groups = lax.axis_size("tp")
    rows, local_width = hidden.shape
    seq_count, head_count, key_width, value_width = carried_state.shape
    proposals = last_keys.shape[1]
    wide_rows = hidden.astype(jnp.float32)
    local_sq = jnp.sum(wide_rows * wide_rows, -1, keepdims=True)
    gain_part = lax.dynamic_slice_in_dim(norm_gain, lax.axis_index("kv") * local_width, local_width)
    scaled = (wide_rows * gain_part.astype(jnp.float32)).astype(jnp.bfloat16)

    def project(weight):
        return jnp.dot(scaled, weight, preferred_element_type=jnp.float32).astype(jnp.bfloat16)

    widths = [w_query.shape[1], w_key.shape[1], w_write.shape[1], w_decay.shape[1], 1]
    spare = -sum(widths) % 128
    first = jnp.concatenate(
        [
            project(w_query),
            project(w_key),
            project(w_write),
            project(w_decay),
            local_sq.astype(jnp.bfloat16),
            jnp.zeros((rows, spare), jnp.bfloat16),
        ],
        -1,
    )
    half = w_gate.shape[1] // 2
    narrow = plane_sum(first, ranks, True)
    proj_value = plane_sum(project(w_value), ranks, False)
    gate_low = plane_sum(project(w_gate[:, :half]), ranks, True)
    gate_high = plane_sum(project(w_gate[:, half:]), ranks, False)
    pieces = []
    begin = 0
    for width in widths:
        pieces.append(narrow[:, begin : begin + width])
        begin += width
    inverse = lax.rsqrt(pieces[4] / (local_width * ranks) + norm_eps)
    proj_gate = jnp.concatenate([gate_low, gate_high], -1) * inverse
    committed = commit(
        decay_rate, carried_state, last_keys, last_values, last_writes, last_decays, accepted
    )
    result = verify_rows(
        pieces[0] * inverse,
        pieces[1] * inverse,
        proj_value * inverse,
        pieces[2] * inverse,
        pieces[3] * inverse,
        decay_rate,
        committed,
    )
    normed = result * lax.rsqrt(jnp.mean(result * result, -1, keepdims=True) + norm_eps) * head_gain
    gated = normed * jax.nn.silu(by_head(proj_gate, seq_count, proposals, value_width))
    gated_rows = (
        jnp.transpose(gated, (0, 2, 1, 3))
        .reshape(seq_count * proposals, head_count * value_width)
        .astype(jnp.bfloat16)
    )
    partial_out = jnp.dot(
        plane_gather(gated_rows, ranks), w_out, preferred_element_type=jnp.float32
    ).astype(jnp.bfloat16)
    shares = lax.all_to_all(
        partial_out.reshape(groups, rows // groups, -1), "tp", 0, 0, tiled=True
    )
    mixed_out = jnp.sum(shares.astype(jnp.float32), 0).astype(jnp.bfloat16)
    return (mixed_out, committed)


def solution(mesh):
    return jax.shard_map(
        per_device,
        mesh=mesh,
        in_specs=(
            P(None, "kv"),
            P(),
            P("kv", "tp"),
            P("kv", "tp"),
            P("kv", "tp"),
            P("kv", "tp"),
            P("kv", "tp"),
            P("kv", "tp"),
            P("tp", "kv"),
            P("tp"),
            P(),
            P("kv", "tp", None, None),
            P("kv", None, "tp"),
            P("kv", None, "tp"),
            P("kv", None, "tp"),
            P("kv", None, "tp"),
            P("kv"),
        ),
        out_specs=(P("tp", "kv"), P("kv", "tp", None, None)),
        check_vma=False,
    )
```
